32 devices in a mesh: grp: 2 (over x), ep: 8 (over z, y), tp: 2 (over core).
Axes of the slice: x: 2, y: 2, z: 4, core: 2. Of those that a mesh axis runs over, the one named last changes fastest.
Arguments:
- tokens: bfloat16 [8192, 2048], P(('grp', 'ep', 'tp')), parts along dimension 0, may hold values from -6 to 6
- norm_gain: float32 [2048], replicated, may hold values from 0.1 to 1.9
- expert_ids: int32 [8192, 2], P(('grp', 'ep', 'tp')), parts along dimension 0, may hold values from 0 to 15, all different within a row; in each aligned block of 256 rows (0 to 255, 256 to 511, ...) at most 64 rows name the same one
- gate_values: float32 [8192, 2], P(('grp', 'ep', 'tp')), parts along dimension 0, may hold values from 0.2 to 2
- w_gate: bfloat16 [16, 2048, 512], P('ep', None, 'tp'), may hold values from -0.125 to 0.125
- w_up: bfloat16 [16, 2048, 512], P('ep', None, 'tp'), may hold values from -0.125 to 0.125
- w_down: bfloat16 [16, 512, 2048], P('ep', 'tp'), may hold values from -0.25 to 0.25
- s_gate: bfloat16 [2048, 512], P(None, 'tp'), may hold values from -0.125 to 0.125
- s_up: bfloat16 [2048, 512], P(None, 'tp'), may hold values from -0.125 to 0.125
- s_down: bfloat16 [512, 2048], P('tp'), may hold values from -0.25 to 0.25
Outputs:
- mixed: bfloat16 [8192, 2048], P(('grp', 'ep', 'tp')), parts along dimension 0
The draws below stay inside these ranges and needn't reach their ends.
There are 2 independent parts, one for each index of `grp`. The reference program is written for one: setup_inputs(seed, part) draws one part's arguments, and reference() takes and returns one part's arrays. A program takes and returns all parts, laid end to end along the dimension named above; an argument that names none is the same for every part. Nothing has to cross between parts.
Inputs may be any that keep to these rules, and one draw needn't show every extreme that they name: `expert_ids`: each row names 2 different experts. Within the rows of one device no expert is named by more than 64 rows, a bound that some block reaches.
All inputs are finite; a program needn't handle non-finite values.
Results may differ from the reference program's by a relative error of at most 0.0068.
Values may be sent and summed in bfloat16 or wider, within the bound.
A program may use at most 128 MiB of HBM per device.

```python
import math
import jax
import jax.numpy as jnp
import numpy as np
from jax import lax

D = 2048
FF = 512
SFF = 512
TOPK = 2
TOK_DEV = 256
EXPERTS = 16
TOKENS = 4096
CAP = 64
N_EP = 8
N_TP = 2


def steps_of(stream_key, dims, shards, low, top_value):
    def one(dim, shards_of):
        heights = jax.random.uniform(jax.random.fold_in(jax.random.fold_in(stream_key, 6), dim), (shards_of,), jnp.float32, low / len(shards), top_value / len(shards))
        return jnp.repeat(jnp.exp(heights), dims[dim] // shards_of).reshape((-1,) + (1,) * (len(dims) - dim - 1))

    loudness = one(*shards[0])
    for cut in shards[1:]:
        loudness = loudness * one(*cut)
    return loudness


def shared_out(key, own, number, rows, amount, top, bound, lean):
    ranking = jax.random.permutation(key, amount)
    heavy_load, common = portions_of(amount, rows * top, bound, lean, True), portions_of(amount, rows * top, bound, lean, False)
    places = jnp.arange(amount)

    def named(tallies, rotation):
        used = int((tallies > 0).sum())
        fixed = max(1, used // 4)
        moved = fixed + (places - fixed + rotation * (used - fixed)) % max(1, amount - fixed)
        return jnp.zeros((amount,), jnp.int32).at[ranking[jnp.where(places < fixed, places, moved)]].set(jnp.asarray(tallies, jnp.int32))

    tallies = jnp.where(number % 4 == 0, named(heavy_load, number // 4), named(common, number - number // 4 - 1))
    mixed = jax.random.permutation(jax.random.fold_in(own, 3), amount)
    donor, taker = mixed[0:amount // 2 * 2:2], mixed[1:amount // 2 * 2:2]
    slack = jnp.minimum(tallies[donor] - 1, bound - tallies[taker]) // 2
    slack = jnp.where((donor == ranking[0]) | (taker == ranking[0]) | (tallies[taker] == 0), 0, jnp.maximum(slack, 0))
    moved = jax.random.randint(jax.random.fold_in(own, 4), (amount // 2,), 0, 1 << 20) % (slack + 1)
    tallies = tallies.at[donor].add(-moved).at[taker].add(moved)
    items = jnp.searchsorted(jnp.cumsum(tallies), jnp.arange(rows * top), side="right").astype(jnp.int32)
    table = items.reshape(top, rows).T
    table = table[jax.random.permutation(jax.random.fold_in(own, 1), rows)]
    rotation = jax.random.randint(jax.random.fold_in(own, 2), (rows, 1), 0, top)
    return jnp.take_along_axis(table, (jnp.arange(top)[None, :] + rotation) % top, axis=1)


def portions_of(count, total, reach, skew, full):
    weights = [(1 << 20) // math.isqrt(grade ** skew) + 1 for grade in range(1, count + 1)]
    largest = reach if full else min(reach, max(-(-total // count), total * weights[0] // sum(weights)))
    least = 1 if total - largest >= count - 1 else 0
    given, rest = [largest] + [least] * (count - 1), total - largest - least * (count - 1)
    while rest > 0:
        free = [i for i in range(1, count) if given[i] < largest] or [i for i in range(1, count) if given[i] < reach]
        mass, remaining = sum([weights[i] for i in free]), rest
        for i in free:
            more = min(reach - given[i], max(1, remaining * weights[i] // mass), rest)
            given[i] = given[i] + more
            rest = rest - more
    return np.array(given)


def normal_values(key, shape, spread, most, shards=(), kind=jnp.bfloat16):
    entries = spread * jax.random.normal(key, shape, jnp.float32)
    if shards:
        entries = entries * steps_of(key, shape, shards, -0.22, 0.18)
    return jnp.clip(entries, -most, most).astype(kind)


def setup_inputs(seed: int = 0, part: int = 0) -> dict:
    key_of = jax.random.split(jax.random.key(seed), 11)
    part_keys = jax.random.split(jax.random.fold_in(key_of[10], part), 11)
    tokens = normal_values(part_keys[0], (TOKENS, D), 1.0, 6.0, ((0, 16),))
    norm_gain = jnp.clip(1.0 + 0.18 * jax.random.normal(key_of[1], (D,), jnp.float32), 0.1, 1.9)
    expert_ids_keys = jax.random.split(jax.random.fold_in(part_keys[2], 1), TOKENS // TOK_DEV)
    expert_ids_turns = jax.random.permutation(jax.random.fold_in(part_keys[2], 3), TOKENS // TOK_DEV)
    expert_ids = jax.vmap(lambda own, number: shared_out(jax.random.fold_in(part_keys[2], 2), own, number, TOK_DEV, EXPERTS, TOPK, CAP, 2))(expert_ids_keys, expert_ids_turns).reshape((TOKENS, TOPK))
    gate_values = jnp.clip(jnp.exp(math.log(2.0) - 2.3025851 * jax.random.uniform(part_keys[3], (TOKENS, TOPK), jnp.float32) ** steps_of(part_keys[3], (TOKENS, TOPK), ((0, 16),), -0.2, 0.2)), 0.2, 2.0)
    w_gate = normal_values(key_of[4], (EXPERTS, D, FF), D ** -0.5, 0.125, ((0, 8), (2, 2)))
    w_up = normal_values(key_of[5], (EXPERTS, D, FF), D ** -0.5, 0.125, ((0, 8), (2, 2)))
    w_down = normal_values(key_of[6], (EXPERTS, FF, D), FF ** -0.5, 0.25, ((0, 8), (1, 2)))
    s_gate = normal_values(key_of[7], (D, SFF), D ** -0.5, 0.125, ((1, 2),))
    s_up = normal_values(key_of[8], (D, SFF), D ** -0.5, 0.125, ((1, 2),))
    s_down = normal_values(key_of[9], (SFF, D), SFF ** -0.5, 0.25, ((0, 2),))
    return dict(tokens=tokens, norm_gain=norm_gain, expert_ids=expert_ids, gate_values=gate_values, w_gate=w_gate, w_up=w_up, w_down=w_down, s_gate=s_gate, s_up=s_up, s_down=s_down)


def reference(tokens, norm_gain, expert_ids, gate_values, w_gate, w_up, w_down, s_gate, s_up, s_down):
    n_tok = tokens.shape[0]
    width = tokens.shape[1]
    topk = expert_ids.shape[1]
    experts_n = w_gate.shape[0]
    xf = tokens.astype(jnp.float32)
    scale = lax.rsqrt(lax.optimization_barrier(jnp.mean(xf * xf, axis=-1, keepdims=True)) + 1e-06)
    normed = (xf * scale * norm_gain.astype(jnp.float32)).astype(jnp.bfloat16)
    s_first = jnp.dot(normed, s_gate, preferred_element_type=jnp.float32)
    s_second = jnp.dot(normed, s_up, preferred_element_type=jnp.float32)
    s_hidden = (jax.nn.silu(s_first) * s_second).astype(jnp.bfloat16)
    shared = jnp.dot(s_hidden, s_down, preferred_element_type=jnp.float32)
    flat_e = expert_ids.reshape(-1).astype(jnp.int32)
    total = flat_e.shape[0]
    order = jnp.argsort(flat_e, stable=True).astype(jnp.int32)
    counts = jnp.bincount(flat_e, length=experts_n).astype(jnp.int32)
    starts = (jnp.cumsum(counts) - counts).astype(jnp.int32)
    most = N_EP * N_TP * CAP
    sorted_tok = jnp.concatenate([(order // topk).astype(jnp.int32), jnp.full((most,), n_tok, jnp.int32)])
    padded = jnp.concatenate([normed, jnp.zeros((1, width), jnp.bfloat16)], axis=0)

    def one_expert(expert):
        index = lax.dynamic_slice(sorted_tok, (starts[expert].astype(jnp.int32),), (most,))
        valid = jnp.arange(most, dtype=jnp.int32) < counts[expert]
        index = jnp.where(valid, index, n_tok).astype(jnp.int32)
        rows = padded[index]
        first = jnp.dot(rows, w_gate[expert], preferred_element_type=jnp.float32)
        second = jnp.dot(rows, w_up[expert], preferred_element_type=jnp.float32)
        hidden = (jax.nn.silu(first) * second).astype(jnp.bfloat16)
        return jnp.dot(hidden, w_down[expert], preferred_element_type=jnp.float32).astype(jnp.bfloat16)
    results = lax.map(one_expert, jnp.arange(experts_n, dtype=jnp.int32))
    inverse = jnp.zeros((total,), jnp.int32).at[order].set(jnp.arange(total, dtype=jnp.int32))
    rank = (inverse - starts[flat_e]).astype(jnp.int32)
    picked = results[flat_e, rank].reshape(n_tok, topk, width)
    routed = lax.optimization_barrier(jnp.sum(gate_values.astype(jnp.float32)[:, :, None] * picked.astype(jnp.float32), axis=1))
    return (shared + routed).astype(jnp.bfloat16)
```

```python
import functools

import jax
import jax.numpy as jnp
from jax import lax
from jax.experimental import pallas as pl
from jax.experimental.pallas import tpu as pltpu
from jax.sharding import PartitionSpec as P

MESH = pl.DeviceIdType.MESH
CHUNKS = 4


def line_shape(ep_size):
    inner = 1
    while (2 * inner) ** 2 <= ep_size:
        inner *= 2
    return ep_size // inner, inner


def dot(a, b):
    return jnp.dot(a, b, preferred_element_type=jnp.float32)


def fused_kernel(
    Z, Y, topk, cap,
    normed, table, wg, wu, wd, sg, su, sd, out,
    blk, tab, arr, sel, res, nres, part, recv, shared,
    G, U, Dn, Gs, Us, Ds,
    lsem, wloc, wsend, wrecv, zsend, zrecv, ysend, yrecv, rsend, rrecv, dsend, drecv,
):
    ep = lax.axis_index("ep")
    tp = lax.axis_index("tp")
    z = ep // Y
    y = ep % Y
    NCH, T, DC = normed.shape
    E = wg.shape[0]
    R = E * cap
    other = 1 - tp

    barrier = pltpu.get_barrier_semaphore()
    pl.semaphore_signal(barrier, inc=1, device_id={"tp": other}, device_id_type=MESH)
    for dz in (1, Z - 1):
        pl.semaphore_signal(
            barrier, inc=1, device_id={"ep": ((z + dz) % Z) * Y + y}, device_id_type=MESH
        )
    for d in range(1, Y):
        pl.semaphore_signal(
            barrier, inc=1, device_id={"ep": z * Y + (y + d) % Y}, device_id_type=MESH
        )

    own_blk = pltpu.make_async_copy(normed, blk.at[z], lsem.at[0])
    own_tab = pltpu.make_async_copy(table, tab.at[z], lsem.at[1])
    own_blk.start()
    own_tab.start()
    weights = ((sg, Gs), (su, Us), (sd, Ds), (wg, G), (wu, U), (wd, Dn))
    local = [
        pltpu.make_async_copy(src, dst.at[tp], wloc.at[i]) for i, (src, dst) in enumerate(weights)
    ]
    for copy in local:
        copy.start()
    own_tab.wait()
    own_blk.wait()
    pl.semaphore_wait(barrier, 3 + Y - 1)

    def z_copy(t, c, way):
        to = {"ep": (z - 1 + 2 * way) * Y + y}
        src, dst = (tab.at[t], tab.at[t]) if c == NCH else (blk.at[t, c], blk.at[t, c])
        return pltpu.make_async_remote_copy(
            src_ref=src, dst_ref=dst, send_sem=zsend.at[way, t, c], recv_sem=zrecv.at[t, c],
            device_id=to, device_id_type=MESH,
        )

    def has_next(way):
        nxt = z - 1 + 2 * way
        return (nxt >= 0) & (nxt < Z)

    for c in (NCH, *range(NCH)):
        for way in range(2):
            @pl.when(has_next(way))
            def _():
                z_copy(z, c, way).start()

    remote = [
        pltpu.make_async_remote_copy(
            src_ref=src, dst_ref=dst.at[tp], send_sem=wsend.at[i], recv_sem=wrecv.at[i],
            device_id={"tp": other}, device_id_type=MESH,
        )
        for i, (src, dst) in enumerate(weights)
    ]
    for copy in remote:
        copy.start()

    row_ids = lax.broadcasted_iota(jnp.int32, (R, T), 0).astype(jnp.float32)

    def spread(t, rank, weighted):
        ids = row_ids + (rank * R).astype(jnp.float32)
        total = jnp.zeros((R, T), jnp.float32)
        for k in range(topk):
            value = tab[t, topk + k : topk + k + 1, :] if weighted else jnp.ones((1, T), jnp.float32)
            total = total + jnp.where(tab[t, k : k + 1, :] == ids, value, 0.0)
        return total.astype(jnp.bfloat16)

    def y_copy(t, d, c):
        return pltpu.make_async_remote_copy(
            src_ref=sel.at[t, d - 1, c], dst_ref=arr.at[t, c, y],
            send_sem=ysend.at[t, d - 1, c], recv_sem=yrecv.at[t, y, c],
            device_id={"ep": z * Y + (y + d) % Y}, device_id_type=MESH,
        )

    def y_arrive(t, d, c):
        from_y = (y + d) % Y
        return pltpu.make_async_remote_copy(
            src_ref=sel.at[t, d - 1, c], dst_ref=arr.at[t, c, from_y],
            send_sem=ysend.at[t, d - 1, c], recv_sem=yrecv.at[t, from_y, c],
            device_id={"ep": z * Y + from_y}, device_id_type=MESH,
        )

    def r_copy(t, d, c):
        to_y = (y + d) % Y
        return pltpu.make_async_remote_copy(
            src_ref=res.at[t, c, to_y], dst_ref=nres.at[t, c, y],
            send_sem=rsend.at[t, d - 1, c], recv_sem=rrecv.at[t, y, c],
            device_id={"ep": z * Y + to_y}, device_id_type=MESH,
        )

    def r_arrive(t, d, c):
        from_y = (y + d) % Y
        return pltpu.make_async_remote_copy(
            src_ref=res.at[t, c, from_y], dst_ref=nres.at[t, c, from_y],
            send_sem=rsend.at[t, d - 1, c], recv_sem=rrecv.at[t, from_y, c],
            device_id={"ep": z * Y + from_y}, device_id_type=MESH,
        )

    def d_copy(t, way, c):
        return pltpu.make_async_remote_copy(
            src_ref=part.at[t, c], dst_ref=recv.at[t + way, c],
            send_sem=dsend.at[t, c], recv_sem=drecv.at[t + way, c],
            device_id={"ep": (z - 1 + 2 * way) * Y + y}, device_id_type=MESH,
        )

    def both(j, body):
        @pl.loop(0, 2)
        def _(way):
            t = z + (2 * way - 1) * j

            @pl.when((t >= 0) & (t < Z))
            def _():
                body(t, way)

    def choose(t, c):
        for d in range(Y):
            picked = dot(spread(t, z * Y + (y + d) % Y, False), blk[t, c]).astype(jnp.bfloat16)
            if d == 0:
                arr[t, c, y] = picked
            else:
                sel[t, d - 1, c] = picked
                y_copy(t, d, c).start()

    def arrive(j, c):
        def body(t, way):
            if c == 0:
                z_copy(t, NCH, 0).wait_recv()
            z_copy(t, c, 0).wait_recv()
            for onward in range(2):
                @pl.when((way == 1 - onward) & has_next(onward))
                def _():
                    if c == 0:
                        z_copy(t, NCH, onward).start()
                    z_copy(t, c, onward).start()
            choose(t, c)

        both(j, body)

    def hidden_of(rows, gate_ref, up_ref):
        first = second = None
        for c in range(NCH):
            g = dot(rows[c], gate_ref[c * DC : (c + 1) * DC, :])
            u = dot(rows[c], up_ref[c * DC : (c + 1) * DC, :])
            first = g if first is None else first + g
            second = u if second is None else second + u
        return (first / (1.0 + jnp.exp(-first)) * second).astype(jnp.bfloat16)

    def experts(t):
        for d in range(1, Y):
            for c in range(NCH):
                y_arrive(t, d, c).wait_recv()

        @pl.loop(0, E)
        def _(e):
            mine = pl.ds(pl.multiple_of(e * cap, cap), cap)
            rows = [arr[t, c, :, mine, :].reshape(Y * cap, DC) for c in range(NCH)]
            halves = [hidden_of(rows, G.at[h, e], U.at[h, e]) for h in range(2)]
            for c in range(NCH):
                cols = slice(c * DC, (c + 1) * DC)
                o = dot(halves[0], Dn[0, e, :, cols]) + dot(halves[1], Dn[1, e, :, cols])
                res[t, c, :, mine, :] = o.astype(jnp.bfloat16).reshape(Y, cap, DC)

        for c in range(NCH):
            for d in range(1, Y):
                r_copy(t, d, c).start()

    def merged(t, c):
        total = None
        for d in range(Y):
            from_y = (y + d) % Y
            if d:
                r_arrive(t, d, c).wait_recv()
            rows = res[t, c, y] if d == 0 else nres[t, c, from_y]
            weight = spread(t, z * Y + from_y, True)
            add = lax.dot_general(
                weight, rows, (((0,), (0,)), ((), ())), preferred_element_type=jnp.float32
            )
            total = add if total is None else total + add
        return total

    def partial(t, way):
        for c in range(NCH):
            part[t, c] = merged(t, c).astype(jnp.bfloat16)

    def pass_on(v):
        for way in range(2):
            t = v - z if way == 1 else 2 * (Z - 1) - z - v
            ok = (t > z) & (t < Z) if way == 1 else (t >= 0) & (t < z)
            upstream = z > 0 if way == 1 else z < Z - 1

            @pl.when(ok)
            def _():
                for c in range(NCH):
                    @pl.when(upstream)
                    def _():
                        d_copy(t, way, c).wait_recv()
                        total = part[t, c].astype(jnp.float32) + recv[t + way, c].astype(jnp.float32)
                        part[t, c] = total.astype(jnp.bfloat16)

                    d_copy(t, way, c).start()

    for c in range(NCH):
        choose(z, c)
    for copy in local[:3]:
        copy.wait()
    for copy in remote[:3]:
        copy.wait_recv()
    rows = [blk[z, c] for c in range(NCH)]
    halves = [hidden_of(rows, Gs.at[h], Us.at[h]) for h in range(2)]
    for c in range(NCH):
        cols = slice(c * DC, (c + 1) * DC)
        shared[c] = dot(halves[0], Ds[0, :, cols]) + dot(halves[1], Ds[1, :, cols])
    for copy in local[3:]:
        copy.wait()
    for copy in remote[3:]:
        copy.wait_recv()

    last = Z - 1
    for j in range(1, Z + 3):
        for c in range(NCH):
            if j <= last:
                arrive(j, c)
            if c == NCH // 2 - 1:
                if j - 1 == 0:
                    experts(z)
                elif j - 1 <= last:
                    both(j - 1, lambda t, way: experts(t))
                if 1 <= j - 2 <= last:
                    both(j - 2, partial)
                    pass_on(j - 2)
    for v in range(Z, 2 * Z - 2):
        pass_on(v)

    for c in range(NCH):
        total = shared[c] + merged(z, c)
        shared[c] = total
        for way, there in ((0, z < Z - 1), (1, z > 0)):
            @pl.when(there)
            def _():
                d_copy(z, way, c).wait_recv()
                shared[c] += recv[z + way, c].astype(jnp.float32)

        out[:, c * DC : (c + 1) * DC] = shared[c].astype(jnp.bfloat16)

    for copy in remote:
        copy.wait_send()
    for way in range(2):
        @pl.when(has_next(way))
        def _():
            @pl.loop(0, Z)
            def _(t):
                @pl.when((t <= z) if way == 1 else (t >= z))
                def _():
                    for c in range(NCH + 1):
                        z_copy(t, c, way).wait_send()

    @pl.loop(0, Z)
    def _(t):
        for c in range(NCH):
            for d in range(1, Y):
                y_copy(t, d, c).wait_send()
                r_copy(t, d, c).wait_send()

        @pl.when(t != z)
        def _():
            for c in range(NCH):
                way = jnp.where(t > z, 1, 0)
                d_copy(t, way, c).wait_send()


def fused(tokens, norm_gain, expert_ids, gate_values, w_gate, w_up, w_down, s_gate, s_up, s_down):
    T, D = tokens.shape
    topk = expert_ids.shape[1]
    ep_size = lax.axis_size("ep")
    E, _, FH = w_gate.shape
    SFH = s_gate.shape[1]
    experts_n = E * ep_size
    cap = 2 * T * topk // experts_n
    Z, Y = line_shape(ep_size)
    NCH = CHUNKS
    DC = D // NCH
    R = E * cap
    bf, f32 = jnp.bfloat16, jnp.float32

    xf = tokens.astype(f32)
    scale = lax.rsqrt(jnp.mean(xf * xf, axis=-1, keepdims=True) + 1e-06)
    normed = (xf * scale * norm_gain).astype(bf).reshape(T, NCH, DC).transpose(1, 0, 2)

    onehot = expert_ids[:, :, None] == jnp.arange(experts_n, dtype=jnp.int32)
    named = jnp.any(onehot, axis=1).astype(bf)
    earlier = (jnp.arange(T)[:, None] > jnp.arange(T)[None, :]).astype(bf)
    before = dot(earlier, named)
    slot = jnp.sum(jnp.where(onehot, before[:, None, :], 0.0), axis=2)
    position = expert_ids.astype(f32) * cap + slot
    table = jnp.concatenate(
        [position.T, gate_values.T, jnp.zeros((8 - 2 * topk, T), f32)], axis=0
    )

    vm, dma = pltpu.VMEM, pltpu.SemaphoreType.DMA
    return pl.pallas_call(
        functools.partial(fused_kernel, Z, Y, topk, cap),
        out_shape=jax.ShapeDtypeStruct((T, D), bf),
        in_specs=[pl.BlockSpec(memory_space=pl.ANY)] * 8,
        out_specs=pl.BlockSpec(memory_space=pltpu.VMEM),
        scratch_shapes=[
            vm((Z, NCH, T, DC), bf),
            vm((Z, 8, T), f32),
            vm((Z, NCH, Y, R, DC), bf),
            vm((Z, Y - 1, NCH, R, DC), bf),
            vm((Z, NCH, Y, R, DC), bf),
            vm((Z, NCH, Y, R, DC), bf),
            vm((Z, NCH, T, DC), bf),
            vm((Z + 1, NCH, T, DC), bf),
            vm((NCH, T, DC), f32),
            vm((2, E, D, FH), bf),
            vm((2, E, D, FH), bf),
            vm((2, E, FH, D), bf),
            vm((2, D, SFH), bf),
            vm((2, D, SFH), bf),
            vm((2, SFH, D), bf),
            dma((2,)),
            dma((6,)),
            dma((6,)),
            dma((6,)),
            dma((2, Z, NCH + 1)),
            dma((Z, NCH + 1)),
            dma((Z, Y - 1, NCH)),
            dma((Z, Y, NCH)),
            dma((Z, Y - 1, NCH)),
            dma((Z, Y, NCH)),
            dma((Z, NCH)),
            dma((Z + 1, NCH)),
        ],
        compiler_params=pltpu.CompilerParams(
            collective_id=0, has_side_effects=True, vmem_limit_bytes=63 * 1024 * 1024
        ),
    )(normed, table, w_gate, w_up, w_down, s_gate, s_up, s_down)


def swiglu_rows(rows, first_w, second_w):
    first = jnp.einsum("xecd,edf->xecf", rows, first_w, preferred_element_type=jnp.float32)
    second = jnp.einsum("xecd,edf->xecf", rows, second_w, preferred_element_type=jnp.float32)
    return (jax.nn.silu(first) * second).astype(jnp.bfloat16)


def shared_swiglu(rows, first_w, second_w):
    first = jnp.dot(rows, first_w, preferred_element_type=jnp.float32)
    second = jnp.dot(rows, second_w, preferred_element_type=jnp.float32)
    return (jax.nn.silu(first) * second).astype(jnp.bfloat16)


def exchanged(tokens, norm_gain, expert_ids, gate_values, w_gate, w_up, w_down, s_gate, s_up, s_down):
    n_rows, width = tokens.shape
    topk = expert_ids.shape[1]
    ep_size = lax.axis_size("ep")
    local_exp = w_gate.shape[0]
    experts_n = local_exp * ep_size
    capacity = 2 * n_rows * topk // experts_n
    xf = tokens.astype(jnp.float32)
    scale = lax.rsqrt(jnp.mean(xf * xf, axis=-1, keepdims=True) + 1e-06)
    normed = (xf * scale * norm_gain).astype(jnp.bfloat16)
    s_hidden = shared_swiglu(lax.all_gather(normed, "tp", axis=0, tiled=True), s_gate, s_up)
    shared = lax.psum_scatter(
        jnp.dot(s_hidden, s_down, preferred_element_type=jnp.float32),
        "tp",
        scatter_dimension=0,
        tiled=True,
    )
    flat_e = expert_ids.reshape(-1)
    onehot = (flat_e[:, None] == jnp.arange(experts_n, dtype=jnp.int32)[None, :]).astype(jnp.int32)
    before = jnp.cumsum(onehot, axis=0) - onehot
    slot = jnp.sum(before * onehot, axis=1)
    position = flat_e * capacity + slot
    flat_tok = jnp.arange(flat_e.shape[0], dtype=jnp.int32) // topk
    slot_tok = jnp.full((experts_n * capacity,), n_rows, jnp.int32).at[position].set(flat_tok)
    padded = jnp.concatenate([normed, jnp.zeros((1, width), jnp.bfloat16)], axis=0)
    outgoing = padded[slot_tok].reshape(ep_size, local_exp, capacity, width)
    arrived = lax.all_to_all(outgoing, "ep", split_axis=0, concat_axis=0, tiled=True)
    full_gate, full_up = (
        lax.all_gather(w_gate, "tp", axis=2, tiled=True),
        lax.all_gather(w_up, "tp", axis=2, tiled=True),
    )
    full_down = lax.all_gather(w_down, "tp", axis=1, tiled=True)
    hidden = swiglu_rows(arrived, full_gate, full_up)
    results = jnp.einsum("xecf,efd->xecd", hidden, full_down, preferred_element_type=jnp.float32)
    returned = lax.all_to_all(
        results.astype(jnp.bfloat16), "ep", split_axis=0, concat_axis=0, tiled=True
    )
    picked = returned.reshape(experts_n * capacity, width)[position].reshape(n_rows, topk, width)
    routed = jnp.sum(gate_values[:, :, None] * picked.astype(jnp.float32), axis=1)
    return (shared + routed).astype(jnp.bfloat16)


def body(tokens, norm_gain, expert_ids, gate_values, w_gate, w_up, w_down, s_gate, s_up, s_down):
    args = (tokens, norm_gain, expert_ids, gate_values, w_gate, w_up, w_down, s_gate, s_up, s_down)
    local_exp = w_gate.shape[0]
    cap = 2 * tokens.shape[0] * expert_ids.shape[1] // (local_exp * lax.axis_size("ep"))
    if cap % 16 == 0 and lax.axis_size("tp") == 2:
        return fused(*args)
    return exchanged(*args)


def solution(mesh):
    return jax.shard_map(
        body,
        mesh=mesh,
        in_specs=(
            P(("grp", "ep", "tp"), None),
            P(),
            P(("grp", "ep", "tp"), None),
            P(("grp", "ep", "tp"), None),
            P("ep", None, "tp"),
            P("ep", None, "tp"),
            P("ep", "tp", None),
            P(None, "tp"),
            P(None, "tp"),
            P("tp", None),
        ),
        out_specs=P(("grp", "ep", "tp"), None),
        check_vma=False,
    )
```

```python
import functools

import jax
import jax.numpy as jnp
from jax import lax
from jax.experimental import pallas as pl
from jax.experimental.pallas import tpu as pltpu
from jax.sharding import PartitionSpec as P

MESH = pl.DeviceIdType.MESH
CHUNKS = 4


def line_shape(ep_size):
    inner = 1
    while (2 * inner) ** 2 <= ep_size:
        inner *= 2
    return ep_size // inner, inner


def dot(a, b):
    return jnp.dot(a, b, preferred_element_type=jnp.float32)


def fused_kernel(
    Z, Y, topk, cap,
    tokens, gain, ids, gates, wg, wu, wd, sg, su, sd, out,
    tok, blk, tab, arr, sel, res, nres, part, recv, shared,
    G, U, Dn, Gs, Us, Ds,
    lsem, wloc, wsend, wrecv, zsend, zrecv, ysend, yrecv, rsend, rrecv, dsend, drecv,
):
    ep = lax.axis_index("ep")
    tp = lax.axis_index("tp")
    z = ep // Y
    y = ep % Y
    T, D = tokens.shape
    NCH = CHUNKS
    DC = D // NCH
    E = wg.shape[0]
    R = E * cap
    other = 1 - tp

    barrier = pltpu.get_barrier_semaphore()
    pl.semaphore_signal(barrier, inc=1, device_id={"tp": other}, device_id_type=MESH)
    for dz in (1, Z - 1):
        pl.semaphore_signal(
            barrier, inc=1, device_id={"ep": ((z + dz) % Z) * Y + y}, device_id_type=MESH
        )
    for d in range(1, Y):
        pl.semaphore_signal(
            barrier, inc=1, device_id={"ep": z * Y + (y + d) % Y}, device_id_type=MESH
        )

    own = pltpu.make_async_copy(tokens, tok, lsem.at[0])
    own.start()
    weights = ((sg, Gs), (su, Us), (sd, Ds), (wg, G), (wu, U), (wd, Dn))
    local = [
        pltpu.make_async_copy(src, dst.at[tp], wloc.at[i]) for i, (src, dst) in enumerate(weights)
    ]
    for copy in local:
        copy.start()

    experts_n = E * Z * Y
    expert = lax.broadcasted_iota(jnp.int32, (experts_n, T), 0).astype(jnp.float32)
    named = ids[...].astype(jnp.float32)
    chosen = [(named[k : k + 1, :] == expert).astype(jnp.float32) for k in range(topk)]
    earlier = lax.broadcasted_iota(jnp.int32, (T, T), 0) < lax.broadcasted_iota(jnp.int32, (T, T), 1)
    before = dot(
        sum(chosen).astype(jnp.bfloat16), jnp.where(earlier, 1.0, 0.0).astype(jnp.bfloat16)
    )
    for k in range(topk):
        slot = jnp.sum(before * chosen[k], axis=0, keepdims=True)
        tab[z, k : k + 1, :] = named[k : k + 1, :] * cap + slot
        tab[z, topk + k : topk + k + 1, :] = gates[k : k + 1, :]
    tab[z, 2 * topk :, :] = jnp.zeros((8 - 2 * topk, T), jnp.float32)

    own.wait()
    step = 16

    @pl.loop(0, T // step)
    def _(i):
        some = pl.ds(pl.multiple_of(i * step, step), step)
        x = tok[some, :].astype(jnp.float32)
        scale = lax.rsqrt(jnp.mean(x * x, axis=-1, keepdims=True) + 1e-06)
        x = (x * scale * gain[...]).astype(jnp.bfloat16)
        for c in range(NCH):
            blk[z, c, some, :] = x[:, c * DC : (c + 1) * DC]

    pl.semaphore_wait(barrier, 3 + Y - 1)

    def z_copy(t, c, way):
        to = {"ep": (z - 1 + 2 * way) * Y + y}
        src, dst = (tab.at[t], tab.at[t]) if c == NCH else (blk.at[t, c], blk.at[t, c])
        return pltpu.make_async_remote_copy(
            src_ref=src, dst_ref=dst, send_sem=zsend.at[way, t, c], recv_sem=zrecv.at[t, c],
            device_id=to, device_id_type=MESH,
        )

    def has_next(way):
        nxt = z - 1 + 2 * way
        return (nxt >= 0) & (nxt < Z)

    for c in (NCH, *range(NCH)):
        for way in range(2):
            @pl.when(has_next(way))
            def _():
                z_copy(z, c, way).start()

    remote = [
        pltpu.make_async_remote_copy(
            src_ref=src, dst_ref=dst.at[tp], send_sem=wsend.at[i], recv_sem=wrecv.at[i],
            device_id={"tp": other}, device_id_type=MESH,
        )
        for i, (src, dst) in enumerate(weights)
    ]
    for copy in remote:
        copy.start()

    row_ids = lax.broadcasted_iota(jnp.int32, (R, T), 0).astype(jnp.float32)

    def spread(t, rank, weighted):
        ids = row_ids + (rank * R).astype(jnp.float32)
        total = jnp.zeros((R, T), jnp.float32)
        for k in range(topk):
            value = tab[t, topk + k : topk + k + 1, :] if weighted else jnp.ones((1, T), jnp.float32)
            total = total + jnp.where(tab[t, k : k + 1, :] == ids, value, 0.0)
        return total.astype(jnp.bfloat16)

    def y_copy(t, d, c):
        return pltpu.make_async_remote_copy(
            src_ref=sel.at[t, d - 1, c], dst_ref=arr.at[t, c, y],
            send_sem=ysend.at[t, d - 1, c], recv_sem=yrecv.at[t, y, c],
            device_id={"ep": z * Y + (y + d) % Y}, device_id_type=MESH,
        )

    def y_arrive(t, d, c):
        from_y = (y + d) % Y
        return pltpu.make_async_remote_copy(
            src_ref=sel.at[t, d - 1, c], dst_ref=arr.at[t, c, from_y],
            send_sem=ysend.at[t, d - 1, c], recv_sem=yrecv.at[t, from_y, c],
            device_id={"ep": z * Y + from_y}, device_id_type=MESH,
        )

    def r_copy(t, d, c):
        to_y = (y + d) % Y
        return pltpu.make_async_remote_copy(
            src_ref=res.at[t, c, to_y], dst_ref=nres.at[t, c, y],
            send_sem=rsend.at[t, d - 1, c], recv_sem=rrecv.at[t, y, c],
            device_id={"ep": z * Y + to_y}, device_id_type=MESH,
        )

    def r_arrive(t, d, c):
        from_y = (y + d) % Y
        return pltpu.make_async_remote_copy(
            src_ref=res.at[t, c, from_y], dst_ref=nres.at[t, c, from_y],
            send_sem=rsend.at[t, d - 1, c], recv_sem=rrecv.at[t, from_y, c],
            device_id={"ep": z * Y + from_y}, device_id_type=MESH,
        )

    def d_copy(t, way, c):
        return pltpu.make_async_remote_copy(
            src_ref=part.at[t, c], dst_ref=recv.at[t + way, c],
            send_sem=dsend.at[t, c], recv_sem=drecv.at[t + way, c],
            device_id={"ep": (z - 1 + 2 * way) * Y + y}, device_id_type=MESH,
        )

    def both(j, body):
        @pl.loop(0, 2)
        def _(way):
            t = z + (2 * way - 1) * j

            @pl.when((t >= 0) & (t < Z))
            def _():
                body(t, way)

    def choose(t, c):
        for d in range(Y):
            picked = dot(spread(t, z * Y + (y + d) % Y, False), blk[t, c]).astype(jnp.bfloat16)
            if d == 0:
                arr[t, c, y] = picked
            else:
                sel[t, d - 1, c] = picked
                y_copy(t, d, c).start()

    def arrive(j, c):
        def body(t, way):
            if c == 0:
                z_copy(t, NCH, 0).wait_recv()
            z_copy(t, c, 0).wait_recv()
            for onward in range(2):
                @pl.when((way == 1 - onward) & has_next(onward))
                def _():
                    if c == 0:
                        z_copy(t, NCH, onward).start()
                    z_copy(t, c, onward).start()
            choose(t, c)

        both(j, body)

    def hidden_of(rows, gate_ref, up_ref):
        first = second = None
        for c in range(NCH):
            g = dot(rows[c], gate_ref[c * DC : (c + 1) * DC, :])
            u = dot(rows[c], up_ref[c * DC : (c + 1) * DC, :])
            first = g if first is None else first + g
            second = u if second is None else second + u
        return (first / (1.0 + jnp.exp(-first)) * second).astype(jnp.bfloat16)

    def experts(t):
        for d in range(1, Y):
            for c in range(NCH):
                y_arrive(t, d, c).wait_recv()

        @pl.loop(0, E)
        def _(e):
            mine = pl.ds(pl.multiple_of(e * cap, cap), cap)
            rows = [arr[t, c, :, mine, :].reshape(Y * cap, DC) for c in range(NCH)]
            halves = [hidden_of(rows, G.at[h, e], U.at[h, e]) for h in range(2)]
            for c in range(NCH):
                cols = slice(c * DC, (c + 1) * DC)
                o = dot(halves[0], Dn[0, e, :, cols]) + dot(halves[1], Dn[1, e, :, cols])
                res[t, c, :, mine, :] = o.astype(jnp.bfloat16).reshape(Y, cap, DC)

        for c in range(NCH):
            for d in range(1, Y):
                r_copy(t, d, c).start()

    def merged(t, c):
        total = None
        for d in range(Y):
            from_y = (y + d) % Y
            if d:
                r_arrive(t, d, c).wait_recv()
            rows = res[t, c, y] if d == 0 else nres[t, c, from_y]
            weight = spread(t, z * Y + from_y, True)
            add = lax.dot_general(
                weight, rows, (((0,), (0,)), ((), ())), preferred_element_type=jnp.float32
            )
            total = add if total is None else total + add
        return total

    def partial(j, c):
        def body(t, way):
            part[t, c] = merged(t, c).astype(jnp.bfloat16)

        both(j, body)

    def pass_on(v, c):
        for way in range(2):
            t = v - z if way == 1 else 2 * (Z - 1) - z - v
            ok = (t > z) & (t < Z) if way == 1 else (t >= 0) & (t < z)
            upstream = z > 0 if way == 1 else z < Z - 1

            @pl.when(ok)
            def _():
                @pl.when(upstream)
                def _():
                    d_copy(t, way, c).wait_recv()
                    total = part[t, c].astype(jnp.float32) + recv[t + way, c].astype(jnp.float32)
                    part[t, c] = total.astype(jnp.bfloat16)

                d_copy(t, way, c).start()

    def finish(c):
        shared[c] += merged(z, c)
        for way, there in ((0, z < Z - 1), (1, z > 0)):
            @pl.when(there)
            def _():
                d_copy(z, way, c).wait_recv()
                shared[c] += recv[z + way, c].astype(jnp.float32)

        out[:, c * DC : (c + 1) * DC] = shared[c].astype(jnp.bfloat16)

    for c in range(NCH):
        choose(z, c)
    for copy in local[:3]:
        copy.wait()
    for copy in remote[:3]:
        copy.wait_recv()
    rows = [blk[z, c] for c in range(NCH)]
    halves = [hidden_of(rows, Gs.at[h], Us.at[h]) for h in range(2)]
    for c in range(NCH):
        cols = slice(c * DC, (c + 1) * DC)
        shared[c] = dot(halves[0], Ds[0, :, cols]) + dot(halves[1], Ds[1, :, cols])
    for copy in local[3:]:
        copy.wait()
    for copy in remote[3:]:
        copy.wait_recv()

    last = Z - 1
    for j in range(1, Z):
        for c in range(NCH):
            arrive(j, c)
            if j == 1 and c == NCH // 2 - 1:
                experts(z)
        if j > 1:
            for c in range(NCH):
                partial(j - 1, c)
                pass_on(j - 1, c)
        both(j, lambda t, way: experts(t))

    for _, v, c in sorted((v + c, v, c) for v in range(last, 2 * Z - 1) for c in range(NCH)):
        if v == last:
            partial(last, c)
        if v < 2 * last:
            pass_on(v, c)
        else:
            finish(c)

    for copy in remote:
        copy.wait_send()
    for way in range(2):
        @pl.when(has_next(way))
        def _():
            @pl.loop(0, Z)
            def _(t):
                @pl.when((t <= z) if way == 1 else (t >= z))
                def _():
                    for c in range(NCH + 1):
                        z_copy(t, c, way).wait_send()

    @pl.loop(0, Z)
    def _(t):
        for c in range(NCH):
            for d in range(1, Y):
                y_copy(t, d, c).wait_send()
                r_copy(t, d, c).wait_send()

        @pl.when(t != z)
        def _():
            for c in range(NCH):
                way = jnp.where(t > z, 1, 0)
                d_copy(t, way, c).wait_send()


def fused(tokens, norm_gain, expert_ids, gate_values, w_gate, w_up, w_down, s_gate, s_up, s_down):
    T, D = tokens.shape
    topk = expert_ids.shape[1]
    ep_size = lax.axis_size("ep")
    E, _, FH = w_gate.shape
    SFH = s_gate.shape[1]
    cap = 2 * T * topk // (E * ep_size)
    Z, Y = line_shape(ep_size)
    NCH = CHUNKS
    DC = D // NCH
    R = E * cap
    bf, f32 = jnp.bfloat16, jnp.float32

    vm, dma = pltpu.VMEM, pltpu.SemaphoreType.DMA
    return pl.pallas_call(
        functools.partial(fused_kernel, Z, Y, topk, cap),
        out_shape=jax.ShapeDtypeStruct((T, D), bf),
        in_specs=[
            pl.BlockSpec(memory_space=pl.ANY),
            pl.BlockSpec(memory_space=pltpu.VMEM),
            pl.BlockSpec(memory_space=pltpu.VMEM),
            pl.BlockSpec(memory_space=pltpu.VMEM),
        ]
        + [pl.BlockSpec(memory_space=pl.ANY)] * 6,
        out_specs=pl.BlockSpec(memory_space=pltpu.VMEM),
        scratch_shapes=[
            vm((T, D), bf),
            vm((Z, NCH, T, DC), bf),
            vm((Z, 8, T), f32),
            vm((Z, NCH, Y, R, DC), bf),
            vm((Z, Y - 1, NCH, R, DC), bf),
            vm((Z, NCH, Y, R, DC), bf),
            vm((Z, NCH, Y, R, DC), bf),
            vm((Z, NCH, T, DC), bf),
            vm((Z + 1, NCH, T, DC), bf),
            vm((NCH, T, DC), f32),
            vm((2, E, D, FH), bf),
            vm((2, E, D, FH), bf),
            vm((2, E, FH, D), bf),
            vm((2, D, SFH), bf),
            vm((2, D, SFH), bf),
            vm((2, SFH, D), bf),
            dma((1,)),
            dma((6,)),
            dma((6,)),
            dma((6,)),
            dma((2, Z, NCH + 1)),
            dma((Z, NCH + 1)),
            dma((Z, Y - 1, NCH)),
            dma((Z, Y, NCH)),
            dma((Z, Y - 1, NCH)),
            dma((Z, Y, NCH)),
            dma((Z, NCH)),
            dma((Z + 1, NCH)),
        ],
        compiler_params=pltpu.CompilerParams(
            collective_id=0, has_side_effects=True, vmem_limit_bytes=63 * 1024 * 1024
        ),
    )(tokens, norm_gain.reshape(1, D), expert_ids.T, gate_values.T, w_gate, w_up, w_down, s_gate, s_up, s_down)


def swiglu_rows(rows, first_w, second_w):
    first = jnp.einsum("xecd,edf->xecf", rows, first_w, preferred_element_type=jnp.float32)
    second = jnp.einsum("xecd,edf->xecf", rows, second_w, preferred_element_type=jnp.float32)
    return (jax.nn.silu(first) * second).astype(jnp.bfloat16)


def shared_swiglu(rows, first_w, second_w):
    first = jnp.dot(rows, first_w, preferred_element_type=jnp.float32)
    second = jnp.dot(rows, second_w, preferred_element_type=jnp.float32)
    return (jax.nn.silu(first) * second).astype(jnp.bfloat16)


def exchanged(tokens, norm_gain, expert_ids, gate_values, w_gate, w_up, w_down, s_gate, s_up, s_down):
    n_rows, width = tokens.shape
    topk = expert_ids.shape[1]
    ep_size = lax.axis_size("ep")
    local_exp = w_gate.shape[0]
    experts_n = local_exp * ep_size
    capacity = 2 * n_rows * topk // experts_n
    xf = tokens.astype(jnp.float32)
    scale = lax.rsqrt(jnp.mean(xf * xf, axis=-1, keepdims=True) + 1e-06)
    normed = (xf * scale * norm_gain).astype(jnp.bfloat16)
    s_hidden = shared_swiglu(lax.all_gather(normed, "tp", axis=0, tiled=True), s_gate, s_up)
    shared = lax.psum_scatter(
        jnp.dot(s_hidden, s_down, preferred_element_type=jnp.float32),
        "tp",
        scatter_dimension=0,
        tiled=True,
    )
    flat_e = expert_ids.reshape(-1)
    onehot = (flat_e[:, None] == jnp.arange(experts_n, dtype=jnp.int32)[None, :]).astype(jnp.int32)
    before = jnp.cumsum(onehot, axis=0) - onehot
    slot = jnp.sum(before * onehot, axis=1)
    position = flat_e * capacity + slot
    flat_tok = jnp.arange(flat_e.shape[0], dtype=jnp.int32) // topk
    slot_tok = jnp.full((experts_n * capacity,), n_rows, jnp.int32).at[position].set(flat_tok)
    padded = jnp.concatenate([normed, jnp.zeros((1, width), jnp.bfloat16)], axis=0)
    outgoing = padded[slot_tok].reshape(ep_size, local_exp, capacity, width)
    arrived = lax.all_to_all(outgoing, "ep", split_axis=0, concat_axis=0, tiled=True)
    full_gate, full_up = (
        lax.all_gather(w_gate, "tp", axis=2, tiled=True),
        lax.all_gather(w_up, "tp", axis=2, tiled=True),
    )
    full_down = lax.all_gather(w_down, "tp", axis=1, tiled=True)
    hidden = swiglu_rows(arrived, full_gate, full_up)
    results = jnp.einsum("xecf,efd->xecd", hidden, full_down, preferred_element_type=jnp.float32)
    returned = lax.all_to_all(
        results.astype(jnp.bfloat16), "ep", split_axis=0, concat_axis=0, tiled=True
    )
    picked = returned.reshape(experts_n * capacity, width)[position].reshape(n_rows, topk, width)
    routed = jnp.sum(gate_values[:, :, None] * picked.astype(jnp.float32), axis=1)
    return (shared + routed).astype(jnp.bfloat16)


def body(tokens, norm_gain, expert_ids, gate_values, w_gate, w_up, w_down, s_gate, s_up, s_down):
    args = (tokens, norm_gain, expert_ids, gate_values, w_gate, w_up, w_down, s_gate, s_up, s_down)
    local_exp = w_gate.shape[0]
    cap = 2 * tokens.shape[0] * expert_ids.shape[1] // (local_exp * lax.axis_size("ep"))
    if cap % 16 == 0 and lax.axis_size("tp") == 2:
        return fused(*args)
    return exchanged(*args)


def solution(mesh):
    return jax.shard_map(
        body,
        mesh=mesh,
        in_specs=(
            P(("grp", "ep", "tp"), None),
            P(),
            P(("grp", "ep", "tp"), None),
            P(("grp", "ep", "tp"), None),
            P("ep", None, "tp"),
            P("ep", None, "tp"),
            P("ep", "tp", None),
            P(None, "tp"),
            P(None, "tp"),
            P("tp", None),
        ),
        out_specs=P(("grp", "ep", "tp"), None),
        check_vma=False,
    )
```
